32 devices in a mesh: grp: 2 (over x), ep: 8 (over z, y), tp: 2 (over core).
Axes of the slice: x: 2, y: 2, z: 4, core: 2. Of those that a mesh axis runs over, the one named last changes fastest.
Arguments:
- tokens: bfloat16 [8192, 2048], P(('grp', 'ep', 'tp')), parts along dimension 0, may hold values from -6 to 6
- norm_gain: float32 [2048], replicated, may hold values from 0.1 to 1.9
- expert_ids: int32 [8192, 2], P(('grp', 'ep', 'tp')), parts along dimension 0, may hold values from 0 to 15, all different within a row; in each aligned block of 256 rows (0 to 255, 256 to 511, ...) at most 64 rows name the same one
- gate_values: float32 [8192, 2], P(('grp', 'ep', 'tp')), parts along dimension 0, may hold values from 0.2 to 2
- w_gate: bfloat16 [16, 2048, 512], P('ep', None, 'tp'), may hold values from -0.125 to 0.125
- w_up: bfloat16 [16, 2048, 512], P('ep', None, 'tp'), may hold values from -0.125 to 0.125
- w_down: bfloat16 [16, 512, 2048], P('ep', 'tp'), may hold values from -0.25 to 0.25
- s_gate: bfloat16 [2048, 512], P(None, 'tp'), may hold values from -0.125 to 0.125
- s_up: bfloat16 [2048, 512], P(None, 'tp'), may hold values from -0.125 to 0.125
- s_down: bfloat16 [512, 2048], P('tp'), may hold values from -0.25 to 0.25
Outputs:
- mixed: bfloat16 [8192, 2048], P(('grp', 'ep', 'tp')), parts along dimension 0
The draws below stay inside these ranges and needn't reach their ends.
There are 2 independent parts, one for each index of `grp`. The reference program is written for one: setup_inputs(seed, part) draws one part's arguments, and reference() takes and returns one part's arrays. A program takes and returns all parts, laid end to end along the dimension named above; an argument that names none is the same for every part. Nothing has to cross between parts.
Inputs may be any that keep to these rules, and one draw needn't show every extreme that they name: `expert_ids`: each row names 2 different experts. Within the rows of one device no expert is named by more than 64 rows, a bound that some block reaches.
All inputs are finite; a program needn't handle non-finite values.
Results may differ from the reference program's by a relative error of at most 0.0068.
Values may be sent and summed in bfloat16 or wider, within the bound.
No kernel may reach another device: no remote copies, remote signals or barrier semaphores. Data moves between devices by JAX's collectives and lax.ppermute only.
A program may use at most 128 MiB of HBM per device.

```python
import math
import jax
import jax.numpy as jnp
import numpy as np
from jax import lax

D = 2048
FF = 512
SFF = 512
TOPK = 2
TOK_DEV = 256
EXPERTS = 16
TOKENS = 4096
CAP = 64
N_EP = 8
N_TP = 2


def steps_of(stream_key, dims, shards, low, top_value):
    def one(dim, shards_of):
        heights = jax.random.uniform(jax.random.fold_in(jax.random.fold_in(stream_key, 6), dim), (shards_of,), jnp.float32, low / len(shards), top_value / len(shards))
        return jnp.repeat(jnp.exp(heights), dims[dim] // shards_of).reshape((-1,) + (1,) * (len(dims) - dim - 1))

    loudness = one(*shards[0])
    for cut in shards[1:]:
        loudness = loudness * one(*cut)
    return loudness


def shared_out(key, own, number, rows, amount, top, bound, lean):
    ranking = jax.random.permutation(key, amount)
    heavy_load, common = portions_of(amount, rows * top, bound, lean, True), portions_of(amount, rows * top, bound, lean, False)
    places = jnp.arange(amount)

    def named(tallies, rotation):
        used = int((tallies > 0).sum())
        fixed = max(1, used // 4)
        moved = fixed + (places - fixed + rotation * (used - fixed)) % max(1, amount - fixed)
        return jnp.zeros((amount,), jnp.int32).at[ranking[jnp.where(places < fixed, places, moved)]].set(jnp.asarray(tallies, jnp.int32))

    tallies = jnp.where(number % 4 == 0, named(heavy_load, number // 4), named(common, number - number // 4 - 1))
    mixed = jax.random.permutation(jax.random.fold_in(own, 3), amount)
    donor, taker = mixed[0:amount // 2 * 2:2], mixed[1:amount // 2 * 2:2]
    slack = jnp.minimum(tallies[donor] - 1, bound - tallies[taker]) // 2
    slack = jnp.where((donor == ranking[0]) | (taker == ranking[0]) | (tallies[taker] == 0), 0, jnp.maximum(slack, 0))
    moved = jax.random.randint(jax.random.fold_in(own, 4), (amount // 2,), 0, 1 << 20) % (slack + 1)
    tallies = tallies.at[donor].add(-moved).at[taker].add(moved)
    items = jnp.searchsorted(jnp.cumsum(tallies), jnp.arange(rows * top), side="right").astype(jnp.int32)
    table = items.reshape(top, rows).T
    table = table[jax.random.permutation(jax.random.fold_in(own, 1), rows)]
    rotation = jax.random.randint(jax.random.fold_in(own, 2), (rows, 1), 0, top)
    return jnp.take_along_axis(table, (jnp.arange(top)[None, :] + rotation) % top, axis=1)


def portions_of(count, total, reach, skew, full):
    weights = [(1 << 20) // math.isqrt(grade ** skew) + 1 for grade in range(1, count + 1)]
    largest = reach if full else min(reach, max(-(-total // count), total * weights[0] // sum(weights)))
    least = 1 if total - largest >= count - 1 else 0
    given, rest = [largest] + [least] * (count - 1), total - largest - least * (count - 1)
    while rest > 0:
        free = [i for i in range(1, count) if given[i] < largest] or [i for i in range(1, count) if given[i] < reach]
        mass, remaining = sum([weights[i] for i in free]), rest
        for i in free:
            more = min(reach - given[i], max(1, remaining * weights[i] // mass), rest)
            given[i] = given[i] + more
            rest = rest - more
    return np.array(given)


def normal_values(key, shape, spread, most, shards=(), kind=jnp.bfloat16):
    entries = spread * jax.random.normal(key, shape, jnp.float32)
    if shards:
        entries = entries * steps_of(key, shape, shards, -0.22, 0.18)
    return jnp.clip(entries, -most, most).astype(kind)


def setup_inputs(seed: int = 0, part: int = 0) -> dict:
    key_of = jax.random.split(jax.random.key(seed), 11)
    part_keys = jax.random.split(jax.random.fold_in(key_of[10], part), 11)
    tokens = normal_values(part_keys[0], (TOKENS, D), 1.0, 6.0, ((0, 16),))
    norm_gain = jnp.clip(1.0 + 0.18 * jax.random.normal(key_of[1], (D,), jnp.float32), 0.1, 1.9)
    expert_ids_keys = jax.random.split(jax.random.fold_in(part_keys[2], 1), TOKENS // TOK_DEV)
    expert_ids_turns = jax.random.permutation(jax.random.fold_in(part_keys[2], 3), TOKENS // TOK_DEV)
    expert_ids = jax.vmap(lambda own, number: shared_out(jax.random.fold_in(part_keys[2], 2), own, number, TOK_DEV, EXPERTS, TOPK, CAP, 2))(expert_ids_keys, expert_ids_turns).reshape((TOKENS, TOPK))
    gate_values = jnp.clip(jnp.exp(math.log(2.0) - 2.3025851 * jax.random.uniform(part_keys[3], (TOKENS, TOPK), jnp.float32) ** steps_of(part_keys[3], (TOKENS, TOPK), ((0, 16),), -0.2, 0.2)), 0.2, 2.0)
    w_gate = normal_values(key_of[4], (EXPERTS, D, FF), D ** -0.5, 0.125, ((0, 8), (2, 2)))
    w_up = normal_values(key_of[5], (EXPERTS, D, FF), D ** -0.5, 0.125, ((0, 8), (2, 2)))
    w_down = normal_values(key_of[6], (EXPERTS, FF, D), FF ** -0.5, 0.25, ((0, 8), (1, 2)))
    s_gate = normal_values(key_of[7], (D, SFF), D ** -0.5, 0.125, ((1, 2),))
    s_up = normal_values(key_of[8], (D, SFF), D ** -0.5, 0.125, ((1, 2),))
    s_down = normal_values(key_of[9], (SFF, D), SFF ** -0.5, 0.25, ((0, 2),))
    return dict(tokens=tokens, norm_gain=norm_gain, expert_ids=expert_ids, gate_values=gate_values, w_gate=w_gate, w_up=w_up, w_down=w_down, s_gate=s_gate, s_up=s_up, s_down=s_down)


def reference(tokens, norm_gain, expert_ids, gate_values, w_gate, w_up, w_down, s_gate, s_up, s_down):
    n_tok = tokens.shape[0]
    width = tokens.shape[1]
    topk = expert_ids.shape[1]
    experts_n = w_gate.shape[0]
    xf = tokens.astype(jnp.float32)
    scale = lax.rsqrt(lax.optimization_barrier(jnp.mean(xf * xf, axis=-1, keepdims=True)) + 1e-06)
    normed = (xf * scale * norm_gain.astype(jnp.float32)).astype(jnp.bfloat16)
    s_first = jnp.dot(normed, s_gate, preferred_element_type=jnp.float32)
    s_second = jnp.dot(normed, s_up, preferred_element_type=jnp.float32)
    s_hidden = (jax.nn.silu(s_first) * s_second).astype(jnp.bfloat16)
    shared = jnp.dot(s_hidden, s_down, preferred_element_type=jnp.float32)
    flat_e = expert_ids.reshape(-1).astype(jnp.int32)
    total = flat_e.shape[0]
    order = jnp.argsort(flat_e, stable=True).astype(jnp.int32)
    counts = jnp.bincount(flat_e, length=experts_n).astype(jnp.int32)
    starts = (jnp.cumsum(counts) - counts).astype(jnp.int32)
    most = N_EP * N_TP * CAP
    sorted_tok = jnp.concatenate([(order // topk).astype(jnp.int32), jnp.full((most,), n_tok, jnp.int32)])
    padded = jnp.concatenate([normed, jnp.zeros((1, width), jnp.bfloat16)], axis=0)

    def one_expert(expert):
        index = lax.dynamic_slice(sorted_tok, (starts[expert].astype(jnp.int32),), (most,))
        valid = jnp.arange(most, dtype=jnp.int32) < counts[expert]
        index = jnp.where(valid, index, n_tok).astype(jnp.int32)
        rows = padded[index]
        first = jnp.dot(rows, w_gate[expert], preferred_element_type=jnp.float32)
        second = jnp.dot(rows, w_up[expert], preferred_element_type=jnp.float32)
        hidden = (jax.nn.silu(first) * second).astype(jnp.bfloat16)
        return jnp.dot(hidden, w_down[expert], preferred_element_type=jnp.float32).astype(jnp.bfloat16)
    results = lax.map(one_expert, jnp.arange(experts_n, dtype=jnp.int32))
    inverse = jnp.zeros((total,), jnp.int32).at[order].set(jnp.arange(total, dtype=jnp.int32))
    rank = (inverse - starts[flat_e]).astype(jnp.int32)
    picked = results[flat_e, rank].reshape(n_tok, topk, width)
    routed = lax.optimization_barrier(jnp.sum(gate_values.astype(jnp.float32)[:, :, None] * picked.astype(jnp.float32), axis=1))
    return (shared + routed).astype(jnp.bfloat16)
```

```python
import functools

import jax
import jax.numpy as jnp
from jax import lax
from jax.experimental import pallas as pl
from jax.experimental.pallas import tpu as pltpu
from jax.sharding import PartitionSpec as P

BF, F32 = jnp.bfloat16, jnp.float32
VMEM_LIMIT = 48 * 1024 * 1024


def cost(flops, nbytes):
    return pl.CostEstimate(flops=int(flops), bytes_accessed=int(nbytes), transcendentals=0)


def norm_rows(tokens, gain):
    n, d = tokens.shape
    step = n // 4

    def kernel(x_ref, g_ref, o_ref):
        x = x_ref[...].astype(F32)
        scale = lax.rsqrt(jnp.mean(x * x, axis=-1, keepdims=True) + 1e-06)
        o_ref[...] = (x * scale * g_ref[...]).astype(BF)

    return pl.pallas_call(
        kernel,
        grid=(n // step,),
        in_specs=[pl.BlockSpec((step, d), lambda i: (i, 0)), pl.BlockSpec((1, d), lambda i: (0, 0))],
        out_specs=pl.BlockSpec((step, d), lambda i: (i, 0)),
        out_shape=jax.ShapeDtypeStruct((n, d), BF),
        cost_estimate=cost(2e9, 2e6),
        name="norm_rows",
    )(tokens, gain.reshape(1, d))


def pick_matrix(keys, first, count, cap):
    n = keys.shape[1]
    slot = lax.broadcasted_iota(jnp.int32, (cap, n), 0).astype(F32)
    return [jnp.broadcast_to(keys[r : r + 1, :], (cap, n)) == slot for r in range(first, first + count)]


def compact(block, keys, local_exp, cap):
    n, d = block.shape
    groups = keys.shape[0] // local_exp
    rows = local_exp * cap

    def kernel(x_ref, k_ref, *outs):
        keys_v = k_ref[...]
        for g in range(groups):
            hits = pick_matrix(keys_v, g * local_exp, local_exp, cap)
            onehot = jnp.concatenate([h.astype(F32) for h in hits], axis=0).astype(BF)
            outs[g][...] = jnp.dot(onehot, x_ref[...], preferred_element_type=F32).astype(BF)

    return pl.pallas_call(
        kernel,
        out_shape=[jax.ShapeDtypeStruct((rows, d), BF)] * groups,
        cost_estimate=cost(2e9, 2 * n * d * 2),
        name="compact_rows",
    )(block, keys)


def combine(keys, weights, parts, local_exp, cap, extra, dtype):
    groups, chunks = len(parts), len(parts[0])
    n = keys.shape[1]
    wide = parts[0][0].shape[1]

    def kernel(k_ref, w_ref, *refs):
        ins, outs = refs[:-chunks], refs[-chunks:]
        keys_v, w_v = k_ref[...], w_ref[...]
        high, low = [], []
        for g in range(groups):
            for j, hit in enumerate(pick_matrix(keys_v, g * local_exp, local_exp, cap)):
                r = g * local_exp + j
                w = jnp.where(hit, jnp.broadcast_to(w_v[r : r + 1, :], hit.shape), 0.0)
                top = w.astype(BF)
                high.append(top)
                low.append((w - top.astype(F32)).astype(BF))
        mat = jnp.concatenate(high + low, axis=0)
        for c in range(chunks):
            rows = jnp.concatenate([ins[g * chunks + c][...] for g in range(groups)], axis=0)
            rows = jnp.concatenate([rows, rows], axis=0)
            total = lax.dot_general(mat, rows, (((0,), (0,)), ((), ())), preferred_element_type=F32)
            if extra is not None:
                total = total + ins[groups * chunks][:, c * wide : (c + 1) * wide]
            outs[c][...] = total.astype(dtype)

    args = [parts[g][c] for g in range(groups) for c in range(chunks)]
    if extra is not None:
        args.append(extra)
    return pl.pallas_call(
        kernel,
        out_shape=[jax.ShapeDtypeStruct((n, wide), dtype)] * chunks,
        compiler_params=pltpu.CompilerParams(vmem_limit_bytes=VMEM_LIMIT),
        cost_estimate=cost(2e9, 2 * n * wide * chunks * 2),
        name="combine_rows",
    )(keys, weights, *args)


def expert_ffn(parts, weights, chunks, dtype):
    local_exp, rows, d = parts[0].shape
    n = len(parts)
    f = weights[0].shape[2]
    wide = d // chunks

    def kernel(*refs):
        ins, (wg, wu, wd, og, ou, od) = refs[:n], refs[n : n + 6]
        outs = refs[n + 6 : n + 6 + n * chunks]
        x_s, acc = refs[n + 6 + n * chunks :]
        half = pl.program_id(1)

        def run(gate, up, down, first):
            x = x_s[...]
            a = jnp.dot(x, gate[0], preferred_element_type=F32)
            b = jnp.dot(x, up[0], preferred_element_type=F32)
            h = ((a / (1.0 + jnp.exp(-a))) * b).astype(BF)
            y = jnp.dot(h, down[0], preferred_element_type=F32)
            if first:
                acc[...] = y
            else:
                y = y + acc[...]
                for i in range(n):
                    for c in range(chunks):
                        piece = y[i * rows : (i + 1) * rows, c * wide : (c + 1) * wide]
                        outs[i * chunks + c][0] = piece.astype(dtype)

        @pl.when(half == 0)
        def _():
            for i in range(n):
                x_s[i * rows : (i + 1) * rows, :] = ins[i][0]
            run(wg, wu, wd, True)

        @pl.when(half == 1)
        def _():
            run(og, ou, od, False)

    def at(shape, late):
        if late:
            return pl.BlockSpec(shape, lambda e, s: (jnp.maximum(e - 1 + s, 0), 0, 0))
        return pl.BlockSpec(shape, lambda e, s: (e, 0, 0))

    return pl.pallas_call(
        kernel,
        grid=(local_exp, 2),
        in_specs=[at((1, rows, d), False)] * n
        + [at((1, d, f), late) if w < 2 else at((1, f, d), late) for late in (False, True) for w in range(3)],
        out_specs=[at((1, rows, wide), False)] * (n * chunks),
        out_shape=[jax.ShapeDtypeStruct((local_exp, rows, wide), dtype)] * (n * chunks),
        scratch_shapes=[pltpu.VMEM((n * rows, d), BF), pltpu.VMEM((n * rows, d), F32)],
        compiler_params=pltpu.CompilerParams(vmem_limit_bytes=VMEM_LIMIT),
        cost_estimate=cost(6e9, 6 * local_exp * d * f * 2),
        name="expert_ffn",
    )(*parts, *weights)


def finish(base, contributions):
    n = base[0].shape[0]
    d = sum(b.shape[1] for b in base)
    step = n // 4
    lists = [base] + contributions
    flat = [a for chunks in lists for a in chunks]

    def kernel(*refs):
        out = refs[-1]
        finest = max(len(c) for c in lists)
        wide = d // finest
        for p in range(finest):
            total, at = None, 0
            for chunks in lists:
                each = d // len(chunks)
                ref = refs[at + p * wide // each]
                low = p * wide % each
                piece = ref[:, low : low + wide].astype(F32)
                total = piece if total is None else total + piece
                at += len(chunks)
            out[:, p * wide : (p + 1) * wide] = total.astype(BF)

    return pl.pallas_call(
        kernel,
        grid=(n // step,),
        in_specs=[pl.BlockSpec((step, a.shape[1]), lambda i: (i, 0)) for a in flat],
        out_specs=pl.BlockSpec((step, d), lambda i: (i, 0)),
        out_shape=jax.ShapeDtypeStruct((n, d), BF),
        cost_estimate=cost(1e9, 6e6),
        name="finish",
    )(*flat)


def body(outer, inner, chunks, tokens, norm_gain, expert_ids, gate_values, w_gate, w_up, w_down, s_gate, s_up, s_down):
    n_rows, width = tokens.shape
    topk = expert_ids.shape[1]
    local_exp = w_gate.shape[0]
    cap = 2 * n_rows * topk // (local_exp * outer * inner)
    half = outer // 2
    me = lax.axis_index("ep")
    z, y = me // inner, me % inner

    def along(pairs):
        return [(a * inner + j, b * inner + j) for a, b in pairs for j in range(inner)]

    def send(x, pairs):
        return lax.ppermute(x, "ep", pairs)

    def across(x, k):
        return send(x, [(i, (i // inner) * inner + (i % inner ^ k)) for i in range(outer * inner)])

    def swap_core(x):
        return lax.ppermute(x, "tp", [(0, 1), (1, 0)])

    slot_block = [list(range(outer))]
    levels = []
    size = 1
    while size < half:
        level = []
        for j in range(size):
            exchange, table = [], [0] * outer
            hops = [[] for _ in range(size - 1)]
            for start in range(0, outer, 2 * size):
                left, right = start + size - 1, start + size
                exchange += [(left, right), (right, left)]
                for d in range(size):
                    table[left - d] = slot_block[j][right]
                    table[right + d] = slot_block[j][left]
                    if d:
                        hops[d - 1] += [(left - d + 1, left - d), (right + d - 1, right + d)]
            level.append((j, exchange, hops, table))
        for entry in level:
            slot_block.append(entry[3])
        levels.append(level)
        size *= 2
    edge = [half - 1 if i < half else half for i in range(outer)]
    away = [-1 if i < half else 1 for i in range(outer)]
    top_block = [[slot_block[j][half if i < half else half - 1] for i in range(outer)] for j in range(half)]
    exchange_top = [(half - 1, half), (half, half - 1)]
    outward = [[(edge[i], edge[i] + away[i] * d) for i in (half - 1, half)] for d in range(half)]
    inward = [[(b, a) for a, b in pairs] for pairs in outward]

    meta = jnp.concatenate([expert_ids.T.astype(F32), gate_values.T], axis=0)
    metas = [meta] + [send(meta, along([(i, i ^ k) for i in range(outer)])) for k in range(1, outer)]

    normed = norm_rows(tokens, norm_gain)

    others = [swap_core(w) for w in (w_gate, w_up, w_down)]
    s_own = [w[None] for w in (s_gate, s_up, s_down)]
    s_others = [swap_core(w)[None] for w in (s_gate, s_up, s_down)]
    routed_w = [w_gate, w_up, w_down] + others

    metas = jnp.stack(metas)

    def meta_of(table):
        return metas[jnp.asarray([i ^ b for i, b in enumerate(table)], jnp.int32)[z]]

    def routing(table, positions):
        m = meta_of(table)
        marks, gates = [], []
        for position in positions:
            for k in range(inner):
                for j in range(local_exp):
                    e = ((position * inner + (y ^ k)) * local_exp + j).astype(F32)
                    same = m[:topk] == e
                    marks.append(jnp.any(same, axis=0))
                    gates.append(jnp.sum(jnp.where(same, m[topk:], 0.0), axis=0))
        return jnp.stack(marks), jnp.stack(gates)

    tables = [routing(table, [z]) for table in slot_block]
    edge_z, away_z = jnp.asarray(edge, jnp.int32)[z], jnp.asarray(away, jnp.int32)[z]
    tables += [routing(table, [edge_z + away_z * d for d in range(half)]) for table in top_block]
    marks = jnp.concatenate([t[0] for t in tables], axis=0)
    gates = jnp.concatenate([t[1] for t in tables], axis=0)
    order = jnp.arange(n_rows)
    earlier = (order[:, None] < order[None, :]).astype(BF)
    rank = jnp.dot(marks.astype(BF), earlier, preferred_element_type=F32)
    keys = jnp.where(marks, rank, -1.0)
    split, at = [], 0
    for t in tables:
        split.append((keys[at : at + t[0].shape[0]], gates[at : at + t[0].shape[0]]))
        at += t[0].shape[0]

    slots = [normed]
    for level in levels:
        for j, exchange, hops, _ in level:
            cur = send(slots[j], along(exchange))
            total = cur
            for pairs in hops:
                cur = send(cur, along(pairs))
                total = total + cur
            slots.append(total)
    tops = [send(slots[j], along(exchange_top)) for j in range(half)]

    def shaped(a):
        return a.reshape(local_exp, cap, width)

    def through_experts(own, for_others):
        got = [across(for_others[k - 1], k) for k in range(1, inner)]
        outs = expert_ffn([shaped(a) for a in [own] + got], routed_w, chunks, BF)
        outs = [a.reshape(local_exp * cap, width // chunks) for a in outs]
        outs = [outs[i * chunks : (i + 1) * chunks] for i in range(inner)]
        return [outs[0]] + [[across(c, k) for c in outs[k]] for k in range(1, inner)]

    shared = expert_ffn([normed[None]], s_own + s_others, 1, F32)[0][0]

    sums = []
    for s, block in enumerate(slots):
        key, gate = split[s]
        rows = compact(block, key, local_exp, cap)
        parts = through_experts(rows[0], rows[1:])
        extra, dtype = (shared, F32) if s == 0 else (None, BF)
        sums.append(combine(key, gate, parts, local_exp, cap, extra, dtype))

    arrived = [[] for _ in slots]
    for j, block in enumerate(tops):
        key, gate = split[len(slots) + j]
        rows = compact(block, key, local_exp, cap)
        mine = list(rows[:inner])
        for d in range(1, half):
            for k in reversed(range(inner)):
                mine[k] = mine[k] + send(rows[d * inner + k], along(outward[d]))
        parts = through_experts(mine[0], mine[1:])
        everything = list(parts)
        for d in range(1, half):
            everything += [[send(c, along(inward[d])) for c in part] for part in parts]
        total = combine(key, gate, everything, local_exp, cap, None, BF)
        arrived[j].append([send(c, along(exchange_top)) for c in total])

    dirty = [set() for _ in slots]
    for j in range(half):
        dirty[j] |= {half - 1, half}

    def plus(a, b):
        return (a.astype(F32) + b.astype(F32)).astype(BF)

    slot = len(slots)
    for level in reversed(levels):
        for j, exchange, hops, _ in reversed(level):
            slot -= 1
            early = sums[slot]
            late = early
            for more in arrived[slot]:
                late = [plus(a, b) for a, b in zip(late, more)]
            changed = dirty[slot]
            for pairs in reversed(hops):
                back = [(b, a) for a, b in pairs]
                late = [plus(c, send(c, along(back))) for c in late]
                changed = changed | {b for _, b in back}
            first = [p for p in exchange if p[0] not in changed]
            rest = [p for p in exchange if p[0] in changed]
            if first:
                arrived[j].append([send(c, along(first)) for c in early])
            if rest:
                arrived[j].append([send(c, along(rest)) for c in late])
            dirty[j] |= {b for _, b in exchange}
    return finish(sums[0], arrived[0])


def solution(mesh):
    ep = mesh.shape["ep"]
    bits = ep.bit_length() - 1
    outer = 1 << ((bits + 1) // 2)
    return jax.shard_map(
        functools.partial(body, outer, ep // outer, 4),
        mesh=mesh,
        in_specs=(
            P(("grp", "ep", "tp"), None),
            P(),
            P(("grp", "ep", "tp"), None),
            P(("grp", "ep", "tp"), None),
            P("ep", None, "tp"),
            P("ep", None, "tp"),
            P("ep", "tp", None),
            P(None, "tp"),
            P(None, "tp"),
            P("tp", None),
        ),
        out_specs=P(("grp", "ep", "tp"), None),
        check_vma=False,
    )
```

```python
import functools

import jax
import jax.numpy as jnp
from jax import lax
from jax.experimental import pallas as pl
from jax.experimental.pallas import tpu as pltpu
from jax.sharding import PartitionSpec as P

BF, F32 = jnp.bfloat16, jnp.float32
VMEM_LIMIT = 48 * 1024 * 1024


def cost(flops, nbytes):
    return pl.CostEstimate(flops=int(flops), bytes_accessed=int(nbytes), transcendentals=0)


def pick_matrix(keys, first, count, cap):
    n = keys.shape[1]
    slot = lax.broadcasted_iota(jnp.int32, (cap, n), 0).astype(F32)
    return [jnp.broadcast_to(keys[r : r + 1, :], (cap, n)) == slot for r in range(first, first + count)]


def compact(block, keys, local_exp, cap):
    n, d = block.shape
    groups = keys.shape[0] // local_exp
    rows = local_exp * cap

    def kernel(x_ref, k_ref, *outs):
        keys_v = k_ref[...]
        for g in range(groups):
            hits = pick_matrix(keys_v, g * local_exp, local_exp, cap)
            onehot = jnp.concatenate([h.astype(F32) for h in hits], axis=0).astype(BF)
            outs[g][...] = jnp.dot(onehot, x_ref[...], preferred_element_type=F32).astype(BF)

    return pl.pallas_call(
        kernel,
        out_shape=[jax.ShapeDtypeStruct((rows, d), BF)] * groups,
        cost_estimate=cost(2e9, 2 * n * d * 2),
        name="compact_rows",
    )(block, keys)


def combine(keys, weights, parts, local_exp, cap, extra, dtype, chunk, chunks):
    groups = len(parts)
    n = keys.shape[1]
    wide = parts[0].shape[1] // chunks

    def kernel(k_ref, w_ref, *refs):
        ins, out = refs[:-1], refs[-1]
        keys_v, w_v = k_ref[...], w_ref[...]
        high, low = [], []
        for r, hit in enumerate(pick_matrix(keys_v, 0, groups * local_exp, cap)):
            w = jnp.where(hit, jnp.broadcast_to(w_v[r : r + 1, :], hit.shape), 0.0)
            top = w.astype(BF)
            high.append(top)
            low.append((w - top.astype(F32)).astype(BF))
        stacked = jnp.concatenate([r[...] for r in ins[:groups]], axis=0)
        mats = [jnp.concatenate(m, axis=0) for m in (high, low)]
        total = None
        for mat in mats:
            piece = lax.dot_general(mat, stacked, (((0,), (0,)), ((), ())), preferred_element_type=F32)
            total = piece if total is None else total + piece
        for more in ins[groups:]:
            total = total + more[...].astype(F32)
        out[...] = total.astype(dtype)

    args = list(parts) + list(extra)

    def at(a):
        if a.shape[1] == wide:
            return pl.BlockSpec((a.shape[0], wide), lambda i: (0, 0))
        return pl.BlockSpec((a.shape[0], wide), lambda i: (0, chunk))

    whole = pl.BlockSpec(keys.shape, lambda i: (0, 0))
    return pl.pallas_call(
        kernel,
        grid=(1,),
        in_specs=[whole, whole] + [at(a) for a in args],
        out_specs=pl.BlockSpec((n, wide), lambda i: (0, 0)),
        out_shape=jax.ShapeDtypeStruct((n, wide), dtype),
        compiler_params=pltpu.CompilerParams(vmem_limit_bytes=VMEM_LIMIT),
        cost_estimate=cost(1.5e9, 2 * n * wide * 2),
        name="combine_rows",
    )(keys, weights, *args)


def expert_ffn(parts, gain, weights, splits, dtype):
    local_exp, rows, d = parts[0].shape
    n = len(parts)
    f = weights[0].shape[2]
    total = sum(splits)

    def kernel(*refs):
        ins, gain_ref, (wg, wu, wd, og, ou, od) = refs[:n], refs[n], refs[n + 1 : n + 7]
        outs = refs[n + 7 : n + 7 + total]
        x_s, acc = refs[n + 7 + total :]
        half = pl.program_id(1)

        def run(gate, up, down, first):
            x = x_s[...]
            a = jnp.dot(x, gate[0], preferred_element_type=F32)
            b = jnp.dot(x, up[0], preferred_element_type=F32)
            h = ((a / (1.0 + jnp.exp(-a))) * b).astype(BF)
            y = jnp.dot(h, down[0], preferred_element_type=F32)
            if first:
                acc[...] = y
            else:
                y = y + acc[...]
                at = 0
                for i in range(n):
                    wide = d // splits[i]
                    for c in range(splits[i]):
                        piece = y[i * rows : (i + 1) * rows, c * wide : (c + 1) * wide]
                        outs[at][0] = piece.astype(dtype)
                        at += 1

        @pl.when(half == 0)
        def _():
            for i in range(n):
                x = ins[i][0].astype(F32)
                scale = lax.rsqrt(jnp.mean(x * x, axis=-1, keepdims=True) + 1e-06)
                x_s[i * rows : (i + 1) * rows, :] = (x * scale * gain_ref[...]).astype(BF)
            run(wg, wu, wd, True)

        @pl.when(half == 1)
        def _():
            run(og, ou, od, False)

    def at(shape, late):
        if late:
            return pl.BlockSpec(shape, lambda e, s: (jnp.maximum(e - 1 + s, 0), 0, 0))
        return pl.BlockSpec(shape, lambda e, s: (e, 0, 0))

    wides = [d // c for c in splits for _ in range(c)]
    return pl.pallas_call(
        kernel,
        grid=(local_exp, 2),
        in_specs=[at((1, rows, d), False)] * n
        + [pl.BlockSpec((1, d), lambda e, s: (0, 0))]
        + [at((1, d, f), late) if w < 2 else at((1, f, d), late) for late in (False, True) for w in range(3)],
        out_specs=[at((1, rows, w), False) for w in wides],
        out_shape=[jax.ShapeDtypeStruct((local_exp, rows, w), dtype) for w in wides],
        scratch_shapes=[pltpu.VMEM((n * rows, d), BF), pltpu.VMEM((n * rows, d), F32)],
        compiler_params=pltpu.CompilerParams(vmem_limit_bytes=VMEM_LIMIT),
        cost_estimate=cost(6e9, 6 * local_exp * d * f * 2),
        name="expert_ffn",
    )(*parts, gain, *weights)


def finish(base, pieces, chunk, chunks, out):
    n, d = base.shape
    wide = d // chunks
    args = [base] + pieces

    def kernel(*refs):
        total = None
        for ref in refs[:-1]:
            v = ref[...].astype(F32)
            total = v if total is None else total + v
        refs[-1][...] = total.astype(BF)

    def at(a):
        if a.shape[1] == wide:
            return pl.BlockSpec((n, wide), lambda i: (0, 0))
        return pl.BlockSpec((n, wide), lambda i: (0, chunk))

    specs = [at(a) for a in args]
    alias = {}
    if out is not None:
        alias = {len(args): 0}
        args = args + [out]
        specs.append(pl.BlockSpec(memory_space=pl.ANY))
        count = len(args) - 1
    else:
        count = len(args)

    def run(*refs):
        kernel(*refs[:count], refs[-1])

    return pl.pallas_call(
        run,
        grid=(1,),
        in_specs=specs,
        out_specs=pl.BlockSpec((n, wide), lambda i: (0, chunk)),
        out_shape=jax.ShapeDtypeStruct((n, d), BF),
        input_output_aliases=alias,
        cost_estimate=cost(1e9, 3e6 / chunks),
        name="finish",
    )(*args)


def body(outer, inner, chunks, tokens, norm_gain, expert_ids, gate_values, w_gate, w_up, w_down, s_gate, s_up, s_down):
    n_rows, width = tokens.shape
    topk = expert_ids.shape[1]
    local_exp = w_gate.shape[0]
    cap = 2 * n_rows * topk // (local_exp * outer * inner)
    half = outer // 2
    me = lax.axis_index("ep")
    z, y = me // inner, me % inner

    def along(pairs):
        return [(a * inner + j, b * inner + j) for a, b in pairs for j in range(inner)]

    def send(x, pairs):
        return lax.ppermute(x, "ep", pairs)

    def across(x, k):
        return send(x, [(i, (i // inner) * inner + (i % inner ^ k)) for i in range(outer * inner)])

    def swap_core(x):
        return lax.ppermute(x, "tp", [(0, 1), (1, 0)])

    slot_block = [list(range(outer))]
    levels = []
    size = 1
    while size < half:
        level = []
        for j in range(size):
            exchange, table = [], [0] * outer
            hops = [[] for _ in range(size - 1)]
            for start in range(0, outer, 2 * size):
                left, right = start + size - 1, start + size
                exchange += [(left, right), (right, left)]
                for d in range(size):
                    table[left - d] = slot_block[j][right]
                    table[right + d] = slot_block[j][left]
                    if d:
                        hops[d - 1] += [(left - d + 1, left - d), (right + d - 1, right + d)]
            level.append((j, exchange, hops, table))
        for entry in level:
            slot_block.append(entry[3])
        levels.append(level)
        size *= 2
    edge = [half - 1 if i < half else half for i in range(outer)]
    away = [-1 if i < half else 1 for i in range(outer)]
    top_block = [[slot_block[j][half if i < half else half - 1] for i in range(outer)] for j in range(half)]
    exchange_top = [(half - 1, half), (half, half - 1)]
    outward = [[(edge[i], edge[i] + away[i] * d) for i in (half - 1, half)] for d in range(half)]
    inward = [[(b, a) for a, b in pairs] for pairs in outward]

    meta = jnp.concatenate([expert_ids.T.astype(F32), gate_values.T], axis=0)
    metas = [meta] + [send(meta, along([(i, i ^ k) for i in range(outer)])) for k in range(1, outer)]

    gain = norm_gain.reshape(1, width)

    others = [swap_core(w) for w in (w_gate, w_up, w_down)]
    s_own = [w[None] for w in (s_gate, s_up, s_down)]
    s_others = [swap_core(w)[None] for w in (s_gate, s_up, s_down)]
    routed_w = [w_gate, w_up, w_down] + others

    metas = jnp.stack(metas)

    def meta_of(table):
        return metas[jnp.asarray([i ^ b for i, b in enumerate(table)], jnp.int32)[z]]

    def routing(table, positions):
        m = meta_of(table)
        marks, gates = [], []
        for position in positions:
            for k in range(inner):
                for j in range(local_exp):
                    e = ((position * inner + (y ^ k)) * local_exp + j).astype(F32)
                    same = m[:topk] == e
                    marks.append(jnp.any(same, axis=0))
                    gates.append(jnp.sum(jnp.where(same, m[topk:], 0.0), axis=0))
        return jnp.stack(marks), jnp.stack(gates)

    tables = [routing(table, [z]) for table in slot_block]
    edge_z, away_z = jnp.asarray(edge, jnp.int32)[z], jnp.asarray(away, jnp.int32)[z]
    tables += [routing(table, [edge_z + away_z * d for d in range(half)]) for table in top_block]
    marks = jnp.concatenate([t[0] for t in tables], axis=0)
    gates = jnp.concatenate([t[1] for t in tables], axis=0)
    order = jnp.arange(n_rows)
    earlier = (order[:, None] < order[None, :]).astype(BF)
    rank = jnp.dot(marks.astype(BF), earlier, preferred_element_type=F32)
    keys = jnp.where(marks, rank, -1.0)
    split, at = [], 0
    for t in tables:
        split.append((keys[at : at + t[0].shape[0]], gates[at : at + t[0].shape[0]]))
        at += t[0].shape[0]

    slots = [tokens]
    for level in levels:
        for j, exchange, hops, _ in level:
            cur = send(slots[j], along(exchange))
            total = cur
            for pairs in hops:
                cur = send(cur, along(pairs))
                total = total + cur
            slots.append(total)
    tops = [send(slots[j], along(exchange_top)) for j in range(half)]

    def shaped(a):
        return a.reshape(local_exp, cap, width)

    def through_experts(own, for_others, split_count):
        got = [across(for_others[k - 1], k) for k in range(1, inner)]
        outs = expert_ffn([shaped(a) for a in [own] + got], gain, routed_w, [split_count] * inner, BF)
        outs = [a.reshape(local_exp * cap, width // split_count) for a in outs]
        outs = [outs[i * split_count : (i + 1) * split_count] for i in range(inner)]
        return [outs[0]] + [[across(c, k) for c in outs[k]] for k in range(1, inner)]

    shared = expert_ffn([tokens[None]], gain, s_own + s_others, [1], F32)[0][0]

    def plus(a, b):
        return (a.astype(F32) + b.astype(F32)).astype(BF)

    sums = []
    for s, block in enumerate(slots):
        key, gate = split[s]
        rows = compact(block, key, local_exp, cap)
        parts = [p[0] for p in through_experts(rows[0], rows[1:], 1)]
        if s == 0:
            sums.append([combine(key, gate, parts, local_exp, cap, [shared], F32, 0, 1)])
        else:
            sums.append([combine(key, gate, parts, local_exp, cap, [], BF, c, chunks) for c in range(chunks)])

    arrived = [[] for _ in slots]
    for j, block in enumerate(tops):
        key, gate = split[len(slots) + j]
        rows = compact(block, key, local_exp, cap)
        mine = list(rows[:inner])
        for d in range(1, half):
            for k in reversed(range(inner)):
                mine[k] = mine[k] + send(rows[d * inner + k], along(outward[d]))
        pieces = 1 if j == 0 else chunks
        parts = through_experts(mine[0], mine[1:], pieces)
        got = []
        for c in range(pieces):
            everything = [p[c] for p in parts]
            for d in range(1, half):
                everything += [send(p[c], along(inward[d])) for p in parts]
            total = combine(key, gate, everything, local_exp, cap, [], BF, 0, 1)
            got.append(send(total, along(exchange_top)))
        arrived[j].append(got)

    slot = len(slots)
    for level in reversed(levels):
        for j, exchange, hops, _ in reversed(level):
            slot -= 1
            late = sums[slot]
            for more in arrived[slot]:
                late = [plus(a, b) for a, b in zip(late, more)]
            for pairs in reversed(hops):
                back = [(b, a) for a, b in pairs]
                late = [plus(c, send(c, along(back))) for c in late]
            arrived[j].append([send(c, along(exchange)) for c in late])
    out = None
    for c in range(chunks):
        pieces = [a[0] if len(a) == 1 else a[c] for a in arrived[0]]
        out = finish(sums[0][0], pieces, c, chunks, out)
    return out


def solution(mesh):
    ep = mesh.shape["ep"]
    bits = ep.bit_length() - 1
    outer = 1 << ((bits + 1) // 2)
    return jax.shard_map(
        functools.partial(body, outer, ep // outer, max(1, 4 // (ep // outer))),
        mesh=mesh,
        in_specs=(
            P(("grp", "ep", "tp"), None),
            P(),
            P(("grp", "ep", "tp"), None),
            P(("grp", "ep", "tp"), None),
            P("ep", None, "tp"),
            P("ep", None, "tp"),
            P("ep", "tp", None),
            P(None, "tp"),
            P(None, "tp"),
            P("tp", None),
        ),
        out_specs=P(("grp", "ep", "tp"), None),
        check_vma=False,
    )
```

```python
import functools

import jax
import jax.numpy as jnp
from jax import lax
from jax.experimental import pallas as pl
from jax.experimental.pallas import tpu as pltpu
from jax.sharding import PartitionSpec as P


CHUNKS = 4
SMALL = pltpu.CompilerParams(vmem_limit_bytes=8 * 1024 * 1024)
LARGE = pltpu.CompilerParams(vmem_limit_bytes=16 * 1024 * 1024)
BF, F32 = jnp.bfloat16, jnp.float32


def cost(flops, nbytes):
    return pl.CostEstimate(flops=int(flops), bytes_accessed=int(nbytes), transcendentals=0)


def route(meta, experts, topk, cap, weighted):
    n = meta.shape[1]
    count = experts.shape[0]
    same = [jnp.broadcast_to(meta[k : k + 1, :], (count, n)) == experts for k in range(topk)]
    marks = functools.reduce(jnp.logical_or, same)
    before = lax.broadcasted_iota(jnp.int32, (n, n), 0) < lax.broadcasted_iota(jnp.int32, (n, n), 1)
    rank = jnp.dot(marks.astype(F32).astype(BF), before.astype(F32).astype(BF), preferred_element_type=F32)
    keys = jnp.where(marks, rank, -1.0)
    slot = lax.broadcasted_iota(jnp.int32, (cap, n), 0).astype(F32)
    hits = [jnp.broadcast_to(keys[r : r + 1, :], (cap, n)) == slot for r in range(count)]
    if not weighted:
        return jnp.concatenate([h.astype(F32) for h in hits], axis=0).astype(BF)
    gates = sum(jnp.where(same[k], jnp.broadcast_to(meta[topk + k : topk + k + 1, :], (count, n)), 0.0) for k in range(topk))
    high, low = [], []
    for r, hit in enumerate(hits):
        w = jnp.where(hit, jnp.broadcast_to(gates[r : r + 1, :], (cap, n)), 0.0)
        top = w.astype(BF)
        high.append(top)
        low.append((w - top.astype(F32)).astype(BF))
    return jnp.concatenate(high, axis=0), jnp.concatenate(low, axis=0)


def compact(block, meta, experts, topk, local_exp, cap):
    n, d = block.shape
    groups = experts.shape[0] // local_exp
    rows = local_exp * cap
    steps = 2
    wide = d // steps

    def kernel(x_ref, m_ref, e_ref, *refs):
        outs, onehot = refs[:-1], refs[-1]

        @pl.when(pl.program_id(0) == 0)
        def _():
            onehot[...] = route(m_ref[...], e_ref[...], topk, cap, False)

        picked = jnp.dot(onehot[...], x_ref[...], preferred_element_type=F32).astype(BF)
        for g in range(groups):
            outs[g][...] = picked[g * rows : (g + 1) * rows]

    return pl.pallas_call(
        kernel,
        grid=(steps,),
        in_specs=[
            pl.BlockSpec((n, wide), lambda i: (0, i)),
            pl.BlockSpec(meta.shape, lambda i: (0, 0)),
            pl.BlockSpec(experts.shape, lambda i: (0, 0)),
        ],
        out_specs=[pl.BlockSpec((rows, wide), lambda i: (0, i))] * groups,
        out_shape=[jax.ShapeDtypeStruct((rows, d), BF)] * groups,
        scratch_shapes=[pltpu.VMEM((groups * rows, n), BF)],
        cost_estimate=cost(2e9, 2 * n * d * 2),
        compiler_params=SMALL,
        name="compact_rows",
    )(block, meta, experts)


def combine(meta, experts, topk, parts, cap, extra, dtype, pieces):
    groups = len(parts)
    n = meta.shape[1]
    d = parts[0].shape[1]
    wide = d // pieces

    def kernel(m_ref, e_ref, *refs):
        ins, outs = refs[:-pieces], refs[-pieces:]
        mats = route(m_ref[...], e_ref[...], topk, cap, True)
        for p in range(pieces):
            low = p * wide
            stacked = jnp.concatenate([r[:, low : low + wide] for r in ins[:groups]], axis=0)
            total = None
            for mat in mats:
                piece = lax.dot_general(mat, stacked, (((0,), (0,)), ((), ())), preferred_element_type=F32)
                total = piece if total is None else total + piece
            for more in ins[groups:]:
                total = total + more[:, low : low + wide].astype(F32)
            outs[p][...] = total.astype(dtype)

    return pl.pallas_call(
        kernel,
        out_shape=[jax.ShapeDtypeStruct((n, wide), dtype)] * pieces,
        cost_estimate=cost(1.5e9, 2 * n * d * 2),
        compiler_params=SMALL,
        name="combine_rows",
    )(meta, experts, *parts, *extra)


def combine_matrix(meta, experts, topk, cap):
    n = meta.shape[1]
    count = experts.shape[0] * cap

    def kernel(m_ref, e_ref, out):
        for i, mat in enumerate(route(m_ref[...], e_ref[...], topk, cap, True)):
            out[:, i * count : (i + 1) * count] = mat.astype(F32).T.astype(BF)

    return pl.pallas_call(
        kernel,
        out_shape=jax.ShapeDtypeStruct((n, 2 * count), BF),
        cost_estimate=cost(1e9, n * count * 4),
        compiler_params=SMALL,
        name="combine_matrix",
    )(meta, experts)


def column_piece(arrays, rows, wide, piece, pieces):
    inside = piece % (pieces // len(arrays))
    return arrays[piece * len(arrays) // pieces], pl.BlockSpec((rows, wide), lambda i: (0, inside))


def combine_piece(matrix, parts, piece, pieces):
    n = matrix.shape[0]
    rows = parts[0][0].shape[0]
    wide = sum(a.shape[1] for a in parts[0]) // pieces

    def kernel(m_ref, *refs):
        stacked = jnp.concatenate([r[...] for r in refs[:-1]], axis=0)
        count = stacked.shape[0]
        total = jnp.dot(m_ref[:, :count], stacked, preferred_element_type=F32)
        total = total + jnp.dot(m_ref[:, count:], stacked, preferred_element_type=F32)
        refs[-1][...] = total.astype(BF)

    args, specs = zip(*[column_piece(p, rows, wide, piece, pieces) for p in parts])
    return pl.pallas_call(
        kernel,
        grid=(1,),
        in_specs=[pl.BlockSpec(matrix.shape, lambda i: (0, 0))] + list(specs),
        out_specs=pl.BlockSpec((n, wide), lambda i: (0, 0)),
        out_shape=jax.ShapeDtypeStruct((n, wide), BF),
        cost_estimate=cost(1e9, n * wide * 8),
        compiler_params=SMALL,
        name="combine_piece",
    )(matrix, *args)


def expert_ffn(parts, gain, weights, splits, dtype):
    local_exp, rows, d = parts[0][0].shape
    n = len(parts)
    flat = [a for p in parts for a in p]
    count = len(flat)
    wides = [d // c for counts in splits for c in counts for _ in range(c)]
    total = len(wides)

    def kernel(*refs):
        x_in, gain_ref, w_in = refs[:count], refs[count], refs[count + 1 : count + 7]
        outs, x_s = refs[count + 7 : count + 7 + total], refs[count + 7 + total]
        for e in range(local_exp):
            at = 0
            for i, group in enumerate(parts):
                x = x_in[at][e].astype(F32)
                for more in range(1, len(group)):
                    x = x + x_in[at + more][e].astype(F32)
                at += len(group)
                scale = lax.rsqrt(jnp.mean(x * x, axis=-1, keepdims=True) + 1e-06)
                low = (e * n + i) * rows
                x_s[low : low + rows, :] = (x * scale * gain_ref[...]).astype(BF)
        for e in range(local_exp):
            x = x_s[e * n * rows : (e + 1) * n * rows, :]
            hidden = []
            for half in range(2):
                gate, up = w_in[3 * half], w_in[3 * half + 1]
                a = jnp.dot(x, gate[e], preferred_element_type=F32)
                b = jnp.dot(x, up[e], preferred_element_type=F32)
                hidden.append(((a / (1.0 + jnp.exp(-a))) * b).astype(BF))
            y = jnp.dot(hidden[0], w_in[2][e], preferred_element_type=F32)
            y = y + jnp.dot(hidden[1], w_in[5][e], preferred_element_type=F32)
            at = 0
            for i in range(n):
                for pieces in splits[i]:
                    wide = d // pieces
                    for c in range(pieces):
                        piece = y[i * rows : (i + 1) * rows, c * wide : (c + 1) * wide]
                        outs[at][e] = piece.astype(dtype)
                        at += 1

    whole = pl.BlockSpec(memory_space=pltpu.VMEM)
    return pl.pallas_call(
        kernel,
        in_specs=[whole] * (count + 7),
        out_specs=[whole] * total,
        out_shape=[jax.ShapeDtypeStruct((local_exp, rows, w), dtype) for w in wides],
        scratch_shapes=[pltpu.VMEM((local_exp * n * rows, d), BF)],
        compiler_params=LARGE,
        cost_estimate=cost(6e9, 6 * weights[0].size * 2),
        name="expert_ffn",
    )(*flat, gain, *weights)


def finish(base, lists, chunk, chunks, out):
    n, d = base.shape
    wide = d // chunks

    args, specs = zip(*[column_piece(arrays, n, wide, chunk, chunks) for arrays in [[base]] + lists])
    args, specs = list(args), list(specs)
    count = len(args)
    alias = {}
    if out is not None:
        alias = {count: 0}
        args.append(out)
        specs.append(pl.BlockSpec(memory_space=pl.ANY))

    def kernel(*refs):
        total = None
        for ref in refs[:count]:
            v = ref[...].astype(F32)
            total = v if total is None else total + v
        refs[-1][...] = total.astype(BF)

    return pl.pallas_call(
        kernel,
        grid=(1,),
        in_specs=specs,
        out_specs=pl.BlockSpec((n, wide), lambda i: (0, chunk)),
        out_shape=jax.ShapeDtypeStruct((n, d), BF),
        input_output_aliases=alias,
        cost_estimate=cost(1e9, 3e6 / chunks),
        compiler_params=SMALL,
        name="finish",
    )(*args)


def body(outer, inner, chunks, tokens, norm_gain, expert_ids, gate_values, w_gate, w_up, w_down, s_gate, s_up, s_down):
    n_rows, width = tokens.shape
    topk = expert_ids.shape[1]
    local_exp = w_gate.shape[0]
    cap = 2 * n_rows * topk // (local_exp * outer * inner)
    half = outer // 2
    me = lax.axis_index("ep")
    z, y = me // inner, me % inner

    def along(pairs):
        return [(a * inner + j, b * inner + j) for a, b in pairs for j in range(inner)]

    def send(x, pairs):
        return lax.ppermute(x, "ep", pairs)

    def across(x, k):
        return send(x, [(i, (i // inner) * inner + (i % inner ^ k)) for i in range(outer * inner)])

    def swap_core(x):
        return lax.ppermute(x, "tp", [(0, 1), (1, 0)])

    slot_block = [list(range(outer))]
    levels = []
    size = 1
    while size < half:
        level = []
        for j in range(size):
            exchange, table = [], [0] * outer
            hops = [[] for _ in range(size - 1)]
            for start in range(0, outer, 2 * size):
                left, right = start + size - 1, start + size
                exchange += [(left, right), (right, left)]
                for d in range(size):
                    table[left - d] = slot_block[j][right]
                    table[right + d] = slot_block[j][left]
                    if d:
                        hops[d - 1] += [(left - d + 1, left - d), (right + d - 1, right + d)]
            level.append((j, exchange, hops, table))
        for entry in level:
            slot_block.append(entry[3])
        levels.append(level)
        size *= 2
    edge = [half - 1 if i < half else half for i in range(outer)]
    away = [-1 if i < half else 1 for i in range(outer)]
    top_block = [[slot_block[j][half if i < half else half - 1] for i in range(outer)] for j in range(half)]
    exchange_top = [(half - 1, half), (half, half - 1)]
    outward = {}
    for d in range(half):
        for k in range(inner):
            pairs = [(edge[i], edge[i] + away[i] * d) for i in (half - 1, half)]
            outward[d, k] = [(a * inner + j, b * inner + (j ^ k)) for a, b in pairs for j in range(inner)]
    inward = {dk: [(b, a) for a, b in pairs] for dk, pairs in outward.items()}

    meta = jnp.concatenate([expert_ids.T.astype(F32), gate_values.T], axis=0)
    gain = norm_gain.reshape(1, width)

    def experts_at(positions):
        bases = [position * inner + (y ^ k) for position in positions for k in range(inner)]
        return jnp.stack([(base * local_exp + j).astype(F32) for base in bases for j in range(local_exp)]).reshape(-1, 1)

    edge_z = jnp.where(z < half, half - 1, half)
    away_z = jnp.where(z < half, -1, 1)
    here = experts_at([z])
    side = experts_at([edge_z + away_z * d for d in range(half)])

    slots, metas = [tokens], [meta]
    for level in levels:
        for j, exchange, hops, _ in level:
            s = len(slots)
            cur, cur_m = send(slots[j], along(exchange)), send(metas[j], along(exchange))
            total, total_m = cur, cur_m
            for pairs in hops:
                cur, cur_m = send(cur, along(pairs)), send(cur_m, along(pairs))
                total, total_m = total + cur, total_m + cur_m
            slots.append(total)
            metas.append(total_m)
    straight = [[(top_block[j][b], b) for b in (half - 1, half)] for j in range(half)]
    top_metas = [send(meta, along(straight[j])) for j in range(half)]
    tops = [send(slots[j], along(exchange_top)) for j in range(half)]

    s_own = [w[None] for w in (s_gate, s_up, s_down)]
    s_others = [swap_core(w)[None] for w in (s_gate, s_up, s_down)]
    routed_w = [w_gate, w_up, w_down] + [swap_core(w) for w in (w_gate, w_up, w_down)]

    def shaped(a):
        return a.reshape(local_exp, cap, width)

    def experts(sources, splits):
        outs = expert_ffn([[shaped(a) for a in part] for part in sources], gain, routed_w, splits, BF)
        outs = [a.reshape(local_exp * cap, a.shape[-1]) for a in outs]
        result, at = [], 0
        for counts in splits:
            result.append([])
            for c in counts:
                result[-1].append(outs[at : at + c])
                at += c
        return result

    shared = expert_ffn([[tokens[None]]], gain, s_own + s_others, [(1,)], F32)[0][0]

    def plus(a, b):
        return (a.astype(F32) + b.astype(F32)).astype(BF)

    sums = []
    for s, block in enumerate(slots):
        rows = compact(block, metas[s], here, topk, local_exp, cap)
        got = [across(rows[k], k) for k in range(1, inner)]
        outs = experts([[rows[0]]] + [[a] for a in got], [(1,)] * inner)
        outs = [o[0][0] for o in outs]
        parts = [outs[0]] + [across(outs[k], k) for k in range(1, inner)]
        if s == 0:
            sums.append(combine(metas[s], here, topk, parts, cap, [shared], F32, 1))
        else:
            sums.append(combine(metas[s], here, topk, parts, cap, [], BF, chunks))

    arrived = [[] for _ in slots]
    for j, block in enumerate(tops):
        rows = compact(block, top_metas[j], side, topk, local_exp, cap)
        matrix = combine_matrix(top_metas[j], side, topk, cap)
        mine = [[rows[0]]] + [[] for _ in range(1, inner)]
        for d in reversed(range(half)):
            for k in reversed(range(inner)):
                if d or k:
                    mine[k].append(send(rows[d * inner + k], outward[d, k]))
        pieces = max(1, chunks // 2) if j == 0 else chunks
        results = experts(mine, [(pieces,)] * inner)
        near = [results[0][0]]
        near += [[across(a, k) for a in results[k][0]] for k in range(1, inner)]
        far = [[send(a, inward[d, 0]) for a in part] for d in range(1, half) for part in near]
        got = []
        for c in range(pieces):
            total = combine_piece(matrix, near + far, c, pieces)
            got.append(send(total, along(exchange_top)))
        arrived[j].append(got)

    slot = len(slots)
    for level in reversed(levels):
        for j, exchange, hops, _ in reversed(level):
            slot -= 1
            late = sums[slot]
            for more in arrived[slot]:
                late = [plus(a, b) for a, b in zip(late, more)]
            for pairs in reversed(hops):
                back = [(b, a) for a, b in pairs]
                late = [plus(a, send(a, along(back))) for a in late]
            arrived[j].append([send(a, along(exchange)) for a in late])
    out = None
    for c in range(chunks):
        out = finish(sums[0][0], arrived[0], c, chunks, out)
    return out


def solution(mesh):
    ep = mesh.shape["ep"]
    bits = ep.bit_length() - 1
    outer = 1 << ((bits + 1) // 2)
    chunks = max(1, CHUNKS * 2 // (ep // outer))

    def layer(*args):
        return body(outer, ep // outer, chunks, *args)

    return jax.shard_map(
        layer,
        mesh=mesh,
        in_specs=(
            P(("grp", "ep", "tp"), None),
            P(),
            P(("grp", "ep", "tp"), None),
            P(("grp", "ep", "tp"), None),
            P("ep", None, "tp"),
            P("ep", None, "tp"),
            P("ep", "tp", None),
            P(None, "tp"),
            P(None, "tp"),
            P("tp", None),
        ),
        out_specs=P(("grp", "ep", "tp"), None),
        check_vma=False,
    )
```

```python
import functools

import jax
import jax.numpy as jnp
from jax import lax
from jax.experimental import pallas as pl
from jax.experimental.pallas import tpu as pltpu
from jax.sharding import PartitionSpec as P


CHUNKS = 4
SMALL = pltpu.CompilerParams(vmem_limit_bytes=8 * 1024 * 1024)
LARGE = pltpu.CompilerParams(vmem_limit_bytes=16 * 1024 * 1024)
BF, F32 = jnp.bfloat16, jnp.float32


def cost(flops, nbytes):
    return pl.CostEstimate(flops=int(flops), bytes_accessed=int(nbytes), transcendentals=0)


def route(meta, experts, topk, cap, weighted):
    n = meta.shape[1]
    count = experts.shape[0]
    same = [jnp.broadcast_to(meta[k : k + 1, :], (count, n)) == experts for k in range(topk)]
    marks = functools.reduce(jnp.logical_or, same)
    before = lax.broadcasted_iota(jnp.int32, (n, n), 0) < lax.broadcasted_iota(jnp.int32, (n, n), 1)
    rank = jnp.dot(marks.astype(F32).astype(BF), before.astype(F32).astype(BF), preferred_element_type=F32)
    keys = jnp.where(marks, rank, -1.0)
    slot = lax.broadcasted_iota(jnp.int32, (cap, n), 0).astype(F32)
    hits = [jnp.broadcast_to(keys[r : r + 1, :], (cap, n)) == slot for r in range(count)]
    if not weighted:
        return jnp.concatenate([h.astype(F32) for h in hits], axis=0).astype(BF)
    gates = sum(jnp.where(same[k], jnp.broadcast_to(meta[topk + k : topk + k + 1, :], (count, n)), 0.0) for k in range(topk))
    high, low = [], []
    for r, hit in enumerate(hits):
        w = jnp.where(hit, jnp.broadcast_to(gates[r : r + 1, :], (cap, n)), 0.0)
        top = w.astype(BF)
        high.append(top)
        low.append((w - top.astype(F32)).astype(BF))
    return jnp.concatenate(high, axis=0), jnp.concatenate(low, axis=0)


def compact(block, meta, experts, topk, local_exp, cap):
    n, d = block.shape
    groups = experts.shape[0] // local_exp
    rows = local_exp * cap
    steps = 2
    wide = d // steps

    def kernel(x_ref, m_ref, e_ref, *refs):
        outs, onehot = refs[:-1], refs[-1]

        @pl.when(pl.program_id(0) == 0)
        def _():
            onehot[...] = route(m_ref[...], e_ref[...], topk, cap, False)

        picked = jnp.dot(onehot[...], x_ref[...], preferred_element_type=F32).astype(BF)
        for g in range(groups):
            outs[g][...] = picked[g * rows : (g + 1) * rows]

    return pl.pallas_call(
        kernel,
        grid=(steps,),
        in_specs=[
            pl.BlockSpec((n, wide), lambda i: (0, i)),
            pl.BlockSpec(meta.shape, lambda i: (0, 0)),
            pl.BlockSpec(experts.shape, lambda i: (0, 0)),
        ],
        out_specs=[pl.BlockSpec((rows, wide), lambda i: (0, i))] * groups,
        out_shape=[jax.ShapeDtypeStruct((rows, d), BF)] * groups,
        scratch_shapes=[pltpu.VMEM((groups * rows, n), BF)],
        cost_estimate=cost(2e9, 2 * n * d * 2),
        compiler_params=SMALL,
        name="compact_rows",
    )(block, meta, experts)


def combine(meta, experts, topk, parts, cap, extra, dtype, pieces):
    groups = len(parts)
    n = meta.shape[1]
    d = parts[0].shape[1]
    wide = d // pieces

    def kernel(m_ref, e_ref, *refs):
        ins, outs = refs[:-pieces], refs[-pieces:]
        mats = route(m_ref[...], e_ref[...], topk, cap, True)
        for p in range(pieces):
            low = p * wide
            stacked = jnp.concatenate([r[:, low : low + wide] for r in ins[:groups]], axis=0)
            total = None
            for mat in mats:
                piece = lax.dot_general(mat, stacked, (((0,), (0,)), ((), ())), preferred_element_type=F32)
                total = piece if total is None else total + piece
            for more in ins[groups:]:
                total = total + more[:, low : low + wide].astype(F32)
            outs[p][...] = total.astype(dtype)

    return pl.pallas_call(
        kernel,
        out_shape=[jax.ShapeDtypeStruct((n, wide), dtype)] * pieces,
        cost_estimate=cost(1.5e9, 2 * n * d * 2),
        compiler_params=SMALL,
        name="combine_rows",
    )(meta, experts, *parts, *extra)


def combine_matrix(meta, experts, topk, cap):
    n = meta.shape[1]
    count = experts.shape[0] * cap

    def kernel(m_ref, e_ref, out):
        for i, mat in enumerate(route(m_ref[...], e_ref[...], topk, cap, True)):
            out[:, i * count : (i + 1) * count] = mat.astype(F32).T.astype(BF)

    return pl.pallas_call(
        kernel,
        out_shape=jax.ShapeDtypeStruct((n, 2 * count), BF),
        cost_estimate=cost(1e9, n * count * 4),
        compiler_params=SMALL,
        name="combine_matrix",
    )(meta, experts)


def column_piece(arrays, rows, wide, piece, pieces):
    inside = piece % (pieces // len(arrays))
    return arrays[piece * len(arrays) // pieces], pl.BlockSpec((rows, wide), lambda i: (0, inside))


def combine_piece(matrix, parts, piece, pieces):
    n = matrix.shape[0]
    rows = parts[0][0].shape[0]
    wide = sum(a.shape[1] for a in parts[0]) // pieces

    def kernel(m_ref, *refs):
        stacked = jnp.concatenate([r[...] for r in refs[:-1]], axis=0)
        count = stacked.shape[0]
        total = jnp.dot(m_ref[:, :count], stacked, preferred_element_type=F32)
        total = total + jnp.dot(m_ref[:, count:], stacked, preferred_element_type=F32)
        refs[-1][...] = total.astype(BF)

    args, specs = zip(*[column_piece(p, rows, wide, piece, pieces) for p in parts])
    return pl.pallas_call(
        kernel,
        grid=(1,),
        in_specs=[pl.BlockSpec(matrix.shape, lambda i: (0, 0))] + list(specs),
        out_specs=pl.BlockSpec((n, wide), lambda i: (0, 0)),
        out_shape=jax.ShapeDtypeStruct((n, wide), BF),
        cost_estimate=cost(1e9, n * wide * 8),
        compiler_params=SMALL,
        name="combine_piece",
    )(matrix, *args)


def expert_ffn(parts, gain, weights, splits, dtype):
    local_exp, rows, d = parts[0][0].shape
    n = len(parts)
    flat = [a for p in parts for a in p]
    count = len(flat)
    wides = [d // c for counts in splits for c in counts for _ in range(c)]
    total = len(wides)

    def kernel(*refs):
        x_in, gain_ref, w_in = refs[:count], refs[count], refs[count + 1 : count + 7]
        outs, x_s = refs[count + 7 : count + 7 + total], refs[count + 7 + total]
        for e in range(local_exp):
            at = 0
            for i, group in enumerate(parts):
                x = x_in[at][e].astype(F32)
                for more in range(1, len(group)):
                    x = x + x_in[at + more][e].astype(F32)
                at += len(group)
                scale = lax.rsqrt(jnp.mean(x * x, axis=-1, keepdims=True) + 1e-06)
                low = (e * n + i) * rows
                x_s[low : low + rows, :] = (x * scale * gain_ref[...]).astype(BF)
        for e in range(local_exp):
            x = x_s[e * n * rows : (e + 1) * n * rows, :]
            hidden = []
            for half in range(2):
                gate, up = w_in[3 * half], w_in[3 * half + 1]
                a = jnp.dot(x, gate[e], preferred_element_type=F32)
                b = jnp.dot(x, up[e], preferred_element_type=F32)
                hidden.append(((a / (1.0 + jnp.exp(-a))) * b).astype(BF))
            y = jnp.dot(hidden[0], w_in[2][e], preferred_element_type=F32)
            y = y + jnp.dot(hidden[1], w_in[5][e], preferred_element_type=F32)
            at = 0
            for i in range(n):
                for pieces in splits[i]:
                    wide = d // pieces
                    for c in range(pieces):
                        piece = y[i * rows : (i + 1) * rows, c * wide : (c + 1) * wide]
                        outs[at][e] = piece.astype(dtype)
                        at += 1

    whole = pl.BlockSpec(memory_space=pltpu.VMEM)
    return pl.pallas_call(
        kernel,
        in_specs=[whole] * (count + 7),
        out_specs=[whole] * total,
        out_shape=[jax.ShapeDtypeStruct((local_exp, rows, w), dtype) for w in wides],
        scratch_shapes=[pltpu.VMEM((local_exp * n * rows, d), BF)],
        compiler_params=LARGE,
        cost_estimate=cost(6e9, 6 * weights[0].size * 2),
        name="expert_ffn",
    )(*flat, gain, *weights)


def finish(base, lists, chunk, chunks, out):
    n, d = base.shape
    wide = d // chunks

    args, specs = zip(*[column_piece(arrays, n, wide, chunk, chunks) for arrays in [[base]] + lists])
    args, specs = list(args), list(specs)
    count = len(args)
    alias = {}
    if out is not None:
        alias = {count: 0}
        args.append(out)
        specs.append(pl.BlockSpec(memory_space=pl.ANY))

    def kernel(*refs):
        total = None
        for ref in refs[:count]:
            v = ref[...].astype(F32)
            total = v if total is None else total + v
        refs[-1][...] = total.astype(BF)

    return pl.pallas_call(
        kernel,
        grid=(1,),
        in_specs=specs,
        out_specs=pl.BlockSpec((n, wide), lambda i: (0, chunk)),
        out_shape=jax.ShapeDtypeStruct((n, d), BF),
        input_output_aliases=alias,
        cost_estimate=cost(1e9, 3e6 / chunks),
        compiler_params=SMALL,
        name="finish",
    )(*args)


def body(outer, inner, chunks, tokens, norm_gain, expert_ids, gate_values, w_gate, w_up, w_down, s_gate, s_up, s_down):
    n_rows, width = tokens.shape
    topk = expert_ids.shape[1]
    local_exp = w_gate.shape[0]
    cap = 2 * n_rows * topk // (local_exp * outer * inner)
    half = outer // 2
    me = lax.axis_index("ep")
    z, y = me // inner, me % inner

    def along(pairs):
        return [(a * inner + j, b * inner + j) for a, b in pairs for j in range(inner)]

    def send(x, pairs):
        return lax.ppermute(x, "ep", pairs)

    def across(x, k):
        return send(x, [(i, (i // inner) * inner + (i % inner ^ k)) for i in range(outer * inner)])

    def swap_core(x):
        return lax.ppermute(x, "tp", [(0, 1), (1, 0)])

    slot_block = [list(range(outer))]
    levels = []
    size = 1
    while size < half:
        level = []
        for j in range(size):
            exchange, table = [], [0] * outer
            hops = [[] for _ in range(size - 1)]
            for start in range(0, outer, 2 * size):
                left, right = start + size - 1, start + size
                exchange += [(left, right), (right, left)]
                for d in range(size):
                    table[left - d] = slot_block[j][right]
                    table[right + d] = slot_block[j][left]
                    if d:
                        hops[d - 1] += [(left - d + 1, left - d), (right + d - 1, right + d)]
            level.append((j, exchange, hops, table))
        for entry in level:
            slot_block.append(entry[3])
        levels.append(level)
        size *= 2
    edge = [half - 1 if i < half else half for i in range(outer)]
    away = [-1 if i < half else 1 for i in range(outer)]
    top_block = [[slot_block[j][half if i < half else half - 1] for i in range(outer)] for j in range(half)]
    exchange_top = [(half - 1, half), (half, half - 1)]
    outward = {}
    for d in range(half):
        for k in range(inner):
            pairs = [(edge[i], edge[i] + away[i] * d) for i in (half - 1, half)]
            outward[d, k] = [(a * inner + j, b * inner + (j ^ k)) for a, b in pairs for j in range(inner)]
    inward = {dk: [(b, a) for a, b in pairs] for dk, pairs in outward.items()}

    meta = jnp.concatenate([expert_ids.T.astype(F32), gate_values.T], axis=0)
    gain = norm_gain.reshape(1, width)

    def experts_at(positions):
        bases = [position * inner + (y ^ k) for position in positions for k in range(inner)]
        return jnp.stack([(base * local_exp + j).astype(F32) for base in bases for j in range(local_exp)]).reshape(-1, 1)

    edge_z = jnp.where(z < half, half - 1, half)
    away_z = jnp.where(z < half, -1, 1)
    here = experts_at([z])
    side = experts_at([edge_z + away_z * d for d in range(half)])

    slots, metas = [tokens], [meta]
    for level in levels:
        for j, exchange, hops, _ in level:
            s = len(slots)
            cur, cur_m = send(slots[j], along(exchange)), send(metas[j], along(exchange))
            total, total_m = cur, cur_m
            for pairs in hops:
                cur, cur_m = send(cur, along(pairs)), send(cur_m, along(pairs))
                total, total_m = total + cur, total_m + cur_m
            slots.append(total)
            metas.append(total_m)
    straight = [[(top_block[j][b], b) for b in (half - 1, half)] for j in range(half)]
    top_metas = [send(meta, along(straight[j])) for j in range(half)]
    tops = [send(slots[j], along(exchange_top)) for j in range(half)]

    s_own = [w[None] for w in (s_gate, s_up, s_down)]
    s_others = [swap_core(w)[None] for w in (s_gate, s_up, s_down)]
    routed_w = [w_gate, w_up, w_down] + [swap_core(w) for w in (w_gate, w_up, w_down)]

    def shaped(a):
        return a.reshape(local_exp, cap, width)

    def experts(sources, splits):
        outs = expert_ffn([[shaped(a) for a in part] for part in sources], gain, routed_w, splits, BF)
        outs = [a.reshape(local_exp * cap, a.shape[-1]) for a in outs]
        result, at = [], 0
        for counts in splits:
            result.append([])
            for c in counts:
                result[-1].append(outs[at : at + c])
                at += c
        return result

    shared = expert_ffn([[tokens[None]]], gain, s_own + s_others, [(1,)], F32)[0][0]

    def plus(a, b):
        return (a.astype(F32) + b.astype(F32)).astype(BF)

    sums = []
    for s, block in enumerate(slots):
        rows = compact(block, metas[s], here, topk, local_exp, cap)
        got = [across(rows[k], k) for k in range(1, inner)]
        outs = experts([[rows[0]]] + [[a] for a in got], [(1,)] * inner)
        outs = [o[0][0] for o in outs]
        parts = [outs[0]] + [across(outs[k], k) for k in range(1, inner)]
        if s == 0:
            sums.append(combine(metas[s], here, topk, parts, cap, [shared], F32, 1))
        else:
            sums.append(combine(metas[s], here, topk, parts, cap, [], BF, chunks))

    arrived = [[] for _ in slots]
    for j, block in enumerate(tops):
        rows = compact(block, top_metas[j], side, topk, local_exp, cap)
        matrix = combine_matrix(top_metas[j], side, topk, cap)
        mine = [[rows[0]]] + [[] for _ in range(1, inner)]
        for d in reversed(range(half)):
            for k in reversed(range(inner)):
                if d or k:
                    mine[k].append(send(rows[d * inner + k], outward[d, k]))
        pieces = max(1, chunks // 2) if j == 0 else chunks
        halves = min(pieces, 2)
        results = experts(mine, [(halves,)] * inner)

        def row(arrays, d, k):
            ends = [edge[i] + away[i] * d for i in (half - 1, half)]
            pairs = [(e * inner + i, e * inner + (i ^ k)) for e in ends for i in range(inner)]
            return [send(a, pairs) for a in arrays]

        near = [results[0][0]] + [row(results[k][0], 0, k) for k in range(1, inner)]
        far = []
        for d in range(1, half):
            crossed = [results[0][0]] + [row(results[k][0], d, k) for k in range(1, inner)]
            for part in crossed:
                far.append([send(a, inward[d, 0]) for a in part])
        got = []
        for c in range(pieces):
            total = combine_piece(matrix, near + far, c, pieces)
            got.append(send(total, along(exchange_top)))
        arrived[j].append(got)

    slot = len(slots)
    for level in reversed(levels):
        for j, exchange, hops, _ in reversed(level):
            slot -= 1
            late = sums[slot]
            for more in arrived[slot]:
                late = [plus(a, b) for a, b in zip(late, more)]
            for pairs in reversed(hops):
                back = [(b, a) for a, b in pairs]
                late = [plus(a, send(a, along(back))) for a in late]
            arrived[j].append([send(a, along(exchange)) for a in late])
    out = None
    for c in range(chunks):
        out = finish(sums[0][0], arrived[0], c, chunks, out)
    return out


def solution(mesh):
    ep = mesh.shape["ep"]
    bits = ep.bit_length() - 1
    outer = 1 << ((bits + 1) // 2)
    chunks = max(1, CHUNKS * 2 // (ep // outer))

    def layer(*args):
        return body(outer, ep // outer, chunks, *args)

    return jax.shard_map(
        layer,
        mesh=mesh,
        in_specs=(
            P(("grp", "ep", "tp"), None),
            P(),
            P(("grp", "ep", "tp"), None),
            P(("grp", "ep", "tp"), None),
            P("ep", None, "tp"),
            P("ep", None, "tp"),
            P("ep", "tp", None),
            P(None, "tp"),
            P(None, "tp"),
            P("tp", None),
        ),
        out_specs=P(("grp", "ep", "tp"), None),
        check_vma=False,
    )
```

```python
import functools

import jax
import jax.numpy as jnp
from jax import lax
from jax.experimental import pallas as pl
from jax.experimental.pallas import tpu as pltpu
from jax.sharding import PartitionSpec as P


CHUNKS = 4
SIDE = 1
SMALL = pltpu.CompilerParams(vmem_limit_bytes=8 * 1024 * 1024)
LARGE = pltpu.CompilerParams(vmem_limit_bytes=16 * 1024 * 1024)
BF, F32 = jnp.bfloat16, jnp.float32


def cost(flops, nbytes):
    return pl.CostEstimate(flops=int(flops), bytes_accessed=int(nbytes), transcendentals=0)


def route(meta, experts, topk, cap, weighted):
    n = meta.shape[1]
    count = experts.shape[0]
    same = [jnp.broadcast_to(meta[k : k + 1, :], (count, n)) == experts for k in range(topk)]
    marks = functools.reduce(jnp.logical_or, same)
    before = lax.broadcasted_iota(jnp.int32, (n, n), 0) < lax.broadcasted_iota(jnp.int32, (n, n), 1)
    rank = jnp.dot(marks.astype(F32).astype(BF), before.astype(F32).astype(BF), preferred_element_type=F32)
    keys = jnp.where(marks, rank, -1.0)
    slot = lax.broadcasted_iota(jnp.int32, (cap, n), 0).astype(F32)
    hits = [jnp.broadcast_to(keys[r : r + 1, :], (cap, n)) == slot for r in range(count)]
    if not weighted:
        return jnp.concatenate([h.astype(F32) for h in hits], axis=0).astype(BF)
    gates = sum(jnp.where(same[k], jnp.broadcast_to(meta[topk + k : topk + k + 1, :], (count, n)), 0.0) for k in range(topk))
    high, low = [], []
    for r, hit in enumerate(hits):
        w = jnp.where(hit, jnp.broadcast_to(gates[r : r + 1, :], (cap, n)), 0.0)
        top = w.astype(BF)
        high.append(top)
        low.append((w - top.astype(F32)).astype(BF))
    return jnp.concatenate(high, axis=0), jnp.concatenate(low, axis=0)


def compact(block, meta, experts, topk, local_exp, cap):
    n, d = block.shape
    groups = experts.shape[0] // local_exp
    rows = local_exp * cap
    steps = 2
    wide = d // steps

    def kernel(x_ref, m_ref, e_ref, *refs):
        outs, onehot = refs[:-1], refs[-1]

        @pl.when(pl.program_id(0) == 0)
        def _():
            onehot[...] = route(m_ref[...], e_ref[...], topk, cap, False)

        picked = jnp.dot(onehot[...], x_ref[...], preferred_element_type=F32).astype(BF)
        for g in range(groups):
            outs[g][...] = picked[g * rows : (g + 1) * rows]

    return pl.pallas_call(
        kernel,
        grid=(steps,),
        in_specs=[
            pl.BlockSpec((n, wide), lambda i: (0, i)),
            pl.BlockSpec(meta.shape, lambda i: (0, 0)),
            pl.BlockSpec(experts.shape, lambda i: (0, 0)),
        ],
        out_specs=[pl.BlockSpec((rows, wide), lambda i: (0, i))] * groups,
        out_shape=[jax.ShapeDtypeStruct((rows, d), BF)] * groups,
        scratch_shapes=[pltpu.VMEM((groups * rows, n), BF)],
        cost_estimate=cost(2e9, 2 * n * d * 2),
        compiler_params=SMALL,
        name="compact_rows",
    )(block, meta, experts)


def combine(meta, experts, topk, parts, cap, extra, dtype, pieces):
    groups = len(parts)
    n = meta.shape[1]
    d = parts[0].shape[1]
    wide = d // pieces

    def kernel(m_ref, e_ref, *refs):
        ins, outs = refs[:-pieces], refs[-pieces:]
        mats = route(m_ref[...], e_ref[...], topk, cap, True)
        for p in range(pieces):
            low = p * wide
            stacked = jnp.concatenate([r[:, low : low + wide] for r in ins[:groups]], axis=0)
            total = None
            for mat in mats:
                piece = lax.dot_general(mat, stacked, (((0,), (0,)), ((), ())), preferred_element_type=F32)
                total = piece if total is None else total + piece
            for more in ins[groups:]:
                total = total + more[:, low : low + wide].astype(F32)
            outs[p][...] = total.astype(dtype)

    return pl.pallas_call(
        kernel,
        out_shape=[jax.ShapeDtypeStruct((n, wide), dtype)] * pieces,
        cost_estimate=cost(1.5e9, 2 * n * d * 2),
        compiler_params=SMALL,
        name="combine_rows",
    )(meta, experts, *parts, *extra)


def combine_matrix(meta, experts, topk, cap):
    n = meta.shape[1]
    count = experts.shape[0] * cap

    def kernel(m_ref, e_ref, out):
        for i, mat in enumerate(route(m_ref[...], e_ref[...], topk, cap, True)):
            out[:, i * count : (i + 1) * count] = mat.astype(F32).T.astype(BF)

    return pl.pallas_call(
        kernel,
        out_shape=jax.ShapeDtypeStruct((n, 2 * count), BF),
        cost_estimate=cost(1e9, n * count * 4),
        compiler_params=SMALL,
        name="combine_matrix",
    )(meta, experts)


def column_piece(arrays, rows, wide, piece):
    low = piece * wide
    for a in arrays:
        if low < a.shape[1]:
            inside = low // wide
            return a, pl.BlockSpec((rows, wide), lambda i: (0, inside))
        low -= a.shape[1]


def combine_piece(matrix, parts, piece, pieces):
    n = matrix.shape[0]
    rows = parts[0][0].shape[0]
    wide = sum(a.shape[1] for a in parts[0]) // pieces

    def kernel(m_ref, *refs):
        stacked = jnp.concatenate([r[...] for r in refs[:-1]], axis=0)
        count = stacked.shape[0]
        total = jnp.dot(m_ref[:, :count], stacked, preferred_element_type=F32)
        total = total + jnp.dot(m_ref[:, count:], stacked, preferred_element_type=F32)
        refs[-1][...] = total.astype(BF)

    args, specs = zip(*[column_piece(p, rows, wide, piece) for p in parts])
    return pl.pallas_call(
        kernel,
        grid=(1,),
        in_specs=[pl.BlockSpec(matrix.shape, lambda i: (0, 0))] + list(specs),
        out_specs=pl.BlockSpec((n, wide), lambda i: (0, 0)),
        out_shape=jax.ShapeDtypeStruct((n, wide), BF),
        cost_estimate=cost(1e9, n * wide * 8),
        compiler_params=SMALL,
        name="combine_piece",
    )(matrix, *args)


def expert_ffn(parts, gain, weights, splits, dtype):
    local_exp, rows, d = parts[0][0].shape
    n = len(parts)
    flat = [a for p in parts for a in p]
    count = len(flat)
    wides = [w for ways in splits for way in ways for w in way]
    total = len(wides)

    def kernel(*refs):
        x_in, gain_ref, w_in = refs[:count], refs[count], refs[count + 1 : count + 7]
        outs, x_s = refs[count + 7 : count + 7 + total], refs[count + 7 + total]
        for e in range(local_exp):
            at = 0
            for i, group in enumerate(parts):
                x = x_in[at][e].astype(F32)
                for more in range(1, len(group)):
                    x = x + x_in[at + more][e].astype(F32)
                at += len(group)
                scale = lax.rsqrt(jnp.mean(x * x, axis=-1, keepdims=True) + 1e-06)
                low = (e * n + i) * rows
                x_s[low : low + rows, :] = (x * scale * gain_ref[...]).astype(BF)
        for e in range(local_exp):
            x = x_s[e * n * rows : (e + 1) * n * rows, :]
            hidden = []
            for half in range(2):
                gate, up = w_in[3 * half], w_in[3 * half + 1]
                a = jnp.dot(x, gate[e], preferred_element_type=F32)
                b = jnp.dot(x, up[e], preferred_element_type=F32)
                hidden.append(((a / (1.0 + jnp.exp(-a))) * b).astype(BF))
            y = jnp.dot(hidden[0], w_in[2][e], preferred_element_type=F32)
            y = y + jnp.dot(hidden[1], w_in[5][e], preferred_element_type=F32)
            at = 0
            for i in range(n):
                for way in splits[i]:
                    low = 0
                    for wide in way:
                        outs[at][e] = y[i * rows : (i + 1) * rows, low : low + wide].astype(dtype)
                        low += wide
                        at += 1

    whole = pl.BlockSpec(memory_space=pltpu.VMEM)
    return pl.pallas_call(
        kernel,
        in_specs=[whole] * (count + 7),
        out_specs=[whole] * total,
        out_shape=[jax.ShapeDtypeStruct((local_exp, rows, w), dtype) for w in wides],
        scratch_shapes=[pltpu.VMEM((local_exp * n * rows, d), BF)],
        compiler_params=LARGE,
        cost_estimate=cost(6e9, 6 * weights[0].size * 2),
        name="expert_ffn",
    )(*flat, gain, *weights)


def finish(base, lists, chunk, chunks, out):
    n, d = base.shape
    wide = d // chunks

    args, specs = zip(*[column_piece(arrays, n, wide, chunk) for arrays in [[base]] + lists])
    args, specs = list(args), list(specs)
    count = len(args)
    alias = {}
    if out is not None:
        alias = {count: 0}
        args.append(out)
        specs.append(pl.BlockSpec(memory_space=pl.ANY))

    def kernel(*refs):
        total = None
        for ref in refs[:count]:
            v = ref[...].astype(F32)
            total = v if total is None else total + v
        refs[-1][...] = total.astype(BF)

    return pl.pallas_call(
        kernel,
        grid=(1,),
        in_specs=specs,
        out_specs=pl.BlockSpec((n, wide), lambda i: (0, chunk)),
        out_shape=jax.ShapeDtypeStruct((n, d), BF),
        input_output_aliases=alias,
        cost_estimate=cost(1e9, 3e6 / chunks),
        compiler_params=SMALL,
        name="finish",
    )(*args)


def body(outer, inner, chunks, tokens, norm_gain, expert_ids, gate_values, w_gate, w_up, w_down, s_gate, s_up, s_down):
    n_rows, width = tokens.shape
    topk = expert_ids.shape[1]
    local_exp = w_gate.shape[0]
    cap = 2 * n_rows * topk // (local_exp * outer * inner)
    half = outer // 2
    me = lax.axis_index("ep")
    z, y = me // inner, me % inner

    def along(pairs):
        return [(a * inner + j, b * inner + j) for a, b in pairs for j in range(inner)]

    def send(x, pairs):
        return lax.ppermute(x, "ep", pairs)

    def across(x, k):
        return send(x, [(i, (i // inner) * inner + (i % inner ^ k)) for i in range(outer * inner)])

    def swap_core(x):
        return lax.ppermute(x, "tp", [(0, 1), (1, 0)])

    slot_block = [list(range(outer))]
    levels = []
    size = 1
    while size < half:
        level = []
        for j in range(size):
            exchange, table = [], [0] * outer
            hops = [[] for _ in range(size - 1)]
            for start in range(0, outer, 2 * size):
                left, right = start + size - 1, start + size
                exchange += [(left, right), (right, left)]
                for d in range(size):
                    table[left - d] = slot_block[j][right]
                    table[right + d] = slot_block[j][left]
                    if d:
                        hops[d - 1] += [(left - d + 1, left - d), (right + d - 1, right + d)]
            level.append((j, exchange, hops, table))
        for entry in level:
            slot_block.append(entry[3])
        levels.append(level)
        size *= 2
    edge = [half - 1 if i < half else half for i in range(outer)]
    away = [-1 if i < half else 1 for i in range(outer)]
    top_block = [[slot_block[j][half if i < half else half - 1] for i in range(outer)] for j in range(half)]
    exchange_top = [(half - 1, half), (half, half - 1)]
    outward = {}
    for d in range(half):
        for k in range(inner):
            pairs = [(edge[i], edge[i] + away[i] * d) for i in (half - 1, half)]
            outward[d, k] = [(a * inner + j, b * inner + (j ^ k)) for a, b in pairs for j in range(inner)]
    inward = {dk: [(b, a) for a, b in pairs] for dk, pairs in outward.items()}

    meta = jnp.concatenate([expert_ids.T.astype(F32), gate_values.T], axis=0)
    gain = norm_gain.reshape(1, width)

    def experts_at(positions):
        bases = [position * inner + (y ^ k) for position in positions for k in range(inner)]
        return jnp.stack([(base * local_exp + j).astype(F32) for base in bases for j in range(local_exp)]).reshape(-1, 1)

    edge_z = jnp.where(z < half, half - 1, half)
    away_z = jnp.where(z < half, -1, 1)
    here = experts_at([z])
    side = experts_at([edge_z + away_z * d for d in range(half)])

    slots, metas = [tokens], [meta]
    for level in levels:
        for j, exchange, hops, _ in level:
            s = len(slots)
            cur, cur_m = send(slots[j], along(exchange)), send(metas[j], along(exchange))
            total, total_m = cur, cur_m
            for pairs in hops:
                cur, cur_m = send(cur, along(pairs)), send(cur_m, along(pairs))
                total, total_m = total + cur, total_m + cur_m
            slots.append(total)
            metas.append(total_m)
    straight = [[(top_block[j][b], b) for b in (half - 1, half)] for j in range(half)]
    top_metas = [send(meta, along(straight[j])) for j in range(half)]
    tops = [send(slots[j], along(exchange_top)) for j in range(half)]

    s_own = [w[None] for w in (s_gate, s_up, s_down)]
    s_others = [swap_core(w)[None] for w in (s_gate, s_up, s_down)]
    routed_w = [w_gate, w_up, w_down] + [swap_core(w) for w in (w_gate, w_up, w_down)]

    def shaped(a):
        return a.reshape(local_exp, cap, width)

    def experts(sources, splits):
        outs = expert_ffn([[shaped(a) for a in part] for part in sources], gain, routed_w, splits, BF)
        outs = [a.reshape(local_exp * cap, a.shape[-1]) for a in outs]
        result, at = [], 0
        for ways in splits:
            result.append([])
            for way in ways:
                result[-1].append(outs[at : at + len(way)])
                at += len(way)
        return result

    shared = expert_ffn([[tokens[None]]], gain, s_own + s_others, [[(width,)]], F32)[0][0]

    def plus(a, b):
        return (a.astype(F32) + b.astype(F32)).astype(BF)

    sums = []
    for s, block in enumerate(slots):
        rows = compact(block, metas[s], here, topk, local_exp, cap)
        got = [across(rows[k], k) for k in range(1, inner)]
        count = 1 if s == 0 else SIDE
        outs = experts([[rows[0]]] + [[a] for a in got], [[(width // count,) * count]] * inner)
        outs = [o[0] for o in outs]
        back = [[across(a, k) for a in outs[k]] for k in range(1, inner)]
        made = []
        for c in range(count):
            parts = [outs[0][c]] + [b[c] for b in back]
            if s == 0:
                made += combine(metas[s], here, topk, parts, cap, [shared], F32, 1)
            else:
                made += combine(metas[s], here, topk, parts, cap, [], BF, chunks // count)
        sums.append(made)

    arrived = [[] for _ in slots]
    for j, block in enumerate(tops):
        rows = compact(block, top_metas[j], side, topk, local_exp, cap)
        matrix = combine_matrix(top_metas[j], side, topk, cap)
        mine = [[rows[0]]] + [[] for _ in range(1, inner)]
        for d in reversed(range(half)):
            for k in reversed(range(inner)):
                if d or k:
                    mine[k].append(send(rows[d * inner + k], outward[d, k]))
        pieces = max(1, chunks // 2) if j == 0 else chunks
        even = (width // min(pieces, 2),) * min(pieces, 2)
        results = experts(mine, [[even]] + [[(width,), even]] * (inner - 1))

        def row(arrays, d, k):
            ends = [edge[i] + away[i] * d for i in (half - 1, half)]
            pairs = [(e * inner + i, e * inner + (i ^ k)) for e in ends for i in range(inner)]
            return [send(a, pairs) for a in arrays]

        near = [results[0][0]] + [row(results[k][0], 0, k) for k in range(1, inner)]
        far = []
        for d in range(1, half):
            crossed = [results[0][0]] + [row(results[k][1], d, k) for k in range(1, inner)]
            for part in crossed:
                far.append([send(a, inward[d, 0]) for a in part])
        got = []
        for c in range(pieces):
            total = combine_piece(matrix, near + far, c, pieces)
            got.append(send(total, along(exchange_top)))
        arrived[j].append(got)

    slot = len(slots)
    for level in reversed(levels):
        for j, exchange, hops, _ in reversed(level):
            slot -= 1
            late = sums[slot]
            for more in arrived[slot]:
                late = [plus(a, b) for a, b in zip(late, more)]
            for pairs in reversed(hops):
                back = [(b, a) for a, b in pairs]
                late = [plus(a, send(a, along(back))) for a in late]
            arrived[j].append([send(a, along(exchange)) for a in late])
    out = None
    for c in range(chunks):
        out = finish(sums[0][0], arrived[0], c, chunks, out)
    return out


def solution(mesh):
    ep = mesh.shape["ep"]
    bits = ep.bit_length() - 1
    outer = 1 << ((bits + 1) // 2)
    chunks = max(1, CHUNKS * 2 // (ep // outer))

    def layer(*args):
        return body(outer, ep // outer, chunks, *args)

    return jax.shard_map(
        layer,
        mesh=mesh,
        in_specs=(
            P(("grp", "ep", "tp"), None),
            P(),
            P(("grp", "ep", "tp"), None),
            P(("grp", "ep", "tp"), None),
            P("ep", None, "tp"),
            P("ep", None, "tp"),
            P("ep", "tp", None),
            P(None, "tp"),
            P(None, "tp"),
            P("tp", None),
        ),
        out_specs=P(("grp", "ep", "tp"), None),
        check_vma=False,
    )
```
